32 devices in a mesh: grp: 2 (over y), fs: 4 (over z), tp: 4 (over x, core).
Axes of the slice: x: 2, y: 2, z: 4, core: 2. Of those that a mesh axis runs over, the one named last changes fastest.
Arguments:
- tokens: bfloat16 [4096, 2048], P(('grp', 'fs')), parts along dimension 0, may hold values from -6 to 6
- pre_gain: float32 [2048], replicated, may hold values from 0.1 to 1.9
- up_weight: float32 [2048, 8192], P('fs', 'tp'), may hold values from -0.125 to 0.125
- up_scale: float32 [8192], P('tp'), may hold values from 0.3 to 3
- down_weight: float32 [8192, 2048], P('tp', 'fs'), may hold values from -0.0625 to 0.0625
- down_scale: float32 [2048], P('fs'), may hold values from 0.3 to 3
- post_gain: float32 [2048], replicated, may hold values from 0.1 to 1.9
Outputs:
- mixed: bfloat16 [4096, 2048], P(('grp', 'fs')), parts along dimension 0
The draws below stay inside these ranges and needn't reach their ends.
There are 2 independent parts, one for each index of `grp`. The reference program is written for one: setup_inputs(seed, part) draws one part's arguments, and reference() takes and returns one part's arrays. A program takes and returns all parts, laid end to end along the dimension named above; an argument that names none is the same for every part. Nothing has to cross between parts.
All inputs are finite; a program needn't handle non-finite values.
Results may differ from the reference program's by a relative error of at most 0.01.
Values may be sent and summed in bfloat16 or wider, within the bound.
No kernel may reach another device: no remote copies, remote signals or barrier semaphores. Data moves between devices by JAX's collectives and lax.ppermute only.
A program may use at most 64 MiB of HBM per device.

```python
import math
import jax
import jax.numpy as jnp
from jax import lax

D = 2048
FF = 8192
TOK_DEV = 512
TOKENS = 2048
N_FS = 4
N_TP = 4


def levels(rng, shape, cuts, least, top_value):
    def one(dim, blocks):
        steps = jax.random.uniform(jax.random.fold_in(jax.random.fold_in(rng, 6), dim), (blocks,), jnp.float32, least / len(cuts), top_value / len(cuts))
        return jnp.repeat(jnp.exp(steps), shape[dim] // blocks).reshape((-1,) + (1,) * (len(shape) - dim - 1))

    gain = one(*cuts[0])
    for cut in cuts[1:]:
        gain = gain * one(*cut)
    return gain


def scatter_about(key, shape, scale, limit, split=(), dtype=jnp.bfloat16):
    gain = levels(key, shape, split, -0.22, 0.18) if split else 1.0
    values = jax.random.normal(key, shape, jnp.float32) * scale * gain
    return jnp.minimum(jnp.maximum(values, -limit), limit).astype(dtype)


def setup_inputs(seed: int = 0, part: int = 0) -> dict:
    seeds = jax.random.split(jax.random.key(seed), 8)
    part_keys = jax.random.split(jax.random.fold_in(seeds[7], part), 8)
    tokens = scatter_about(part_keys[0], (TOKENS, D), 1.0, 6.0, ((0, 4),))
    pre_gain = jnp.clip(1.0 + 0.18 * jax.random.normal(seeds[1], (D,), jnp.float32), 0.1, 1.9)
    up_weight = scatter_about(seeds[2], (D, FF), D ** -0.5, 0.125, ((0, 4), (1, 4)), jnp.float32)
    up_scale = jnp.clip(jnp.exp(math.log(3.0) - 2.3025851 * jax.random.uniform(seeds[3], (FF,), jnp.float32) ** levels(seeds[3], (FF,), ((0, 4),), -0.2, 0.2)), 0.3, 3.0)
    down_weight = scatter_about(seeds[4], (FF, D), FF ** -0.5, 0.0625, ((0, 4), (1, 4)), jnp.float32)
    down_scale = jnp.clip(jnp.exp(math.log(3.0) - 2.3025851 * jax.random.uniform(seeds[5], (D,), jnp.float32) ** levels(seeds[5], (D,), ((0, 4),), -0.2, 0.2)), 0.3, 3.0)
    post_gain = jnp.clip(1.0 + 0.18 * jax.random.normal(seeds[6], (D,), jnp.float32), 0.1, 1.9)
    return {"tokens": tokens, "pre_gain": pre_gain, "up_weight": up_weight, "up_scale": up_scale, "down_weight": down_weight, "down_scale": down_scale, "post_gain": post_gain}


epsilon = 1e-06

def rms_rows(values, scaling):
    return values * lax.rsqrt(lax.optimization_barrier(jnp.mean(values * values, axis=-1, keepdims=True)) + epsilon) * scaling

def reference(tokens, pre_gain, up_weight, up_scale, down_weight, down_scale, post_gain):
    up_cast = up_weight.astype(jnp.bfloat16)
    down_cast = down_weight.astype(jnp.bfloat16)
    block_width = FF // N_TP

    def row_block(rows):
        residual = rows.astype(jnp.float32)
        normed = rms_rows(residual, pre_gain).astype(jnp.bfloat16)
        lifted = jnp.dot(normed, up_cast, preferred_element_type=jnp.float32) * up_scale
        hidden = jnp.square(jax.nn.relu(lifted)).astype(jnp.bfloat16)
        running = jnp.zeros((rows.shape[0], D), jnp.float32)
        for member in range(N_TP):
            low = member * block_width
            high = low + block_width
            partial_value = jnp.dot(hidden[:, low:high], down_cast[low:high], preferred_element_type=jnp.float32) * down_scale
            partial_value = lax.optimization_barrier(partial_value.astype(jnp.bfloat16))
            running = running + partial_value.astype(jnp.float32)
        branch = lax.optimization_barrier(running.astype(jnp.bfloat16)).astype(jnp.float32)
        return (residual + rms_rows(branch, post_gain)).astype(jnp.bfloat16)
    result = lax.map(row_block, tokens.reshape(N_FS, TOK_DEV, D))
    return result.reshape(N_FS * TOK_DEV, D)
```

```python
import jax
import jax.numpy as jnp
from jax import lax
from jax.sharding import PartitionSpec as P

epsilon = 1e-06
CORES = 2


def rms_rows(values, scaling):
    return values * lax.rsqrt(jnp.mean(values * values, axis=-1, keepdims=True) + epsilon) * scaling


def pieces_of(width):
    return 2 if width % 256 == 0 else 1


def after(value, *earlier):
    return lax.optimization_barrier((value,) + earlier)[0]


def solution(mesh):
    n_grp, n_fs, n_tp = (mesh.shape[name] for name in ("grp", "fs", "tp"))
    n_x = n_tp // CORES
    ring = [(i, (i + 1) % n_fs) for i in range(n_fs)]
    swap_core = [(t, t ^ 1) for t in range(n_tp)]

    def grp_shift(s):
        return [(g, (g + s) % n_grp) for g in range(n_grp)]

    def x_shift(s):
        return [(t, (t + CORES * s) % n_tp) for t in range(n_tp)]

    def on_device(tokens, pre_gain, up_weight, up_scale, down_weight, down_scale, post_gain):
        grp, fs, tp = lax.axis_index("grp"), lax.axis_index("fs"), lax.axis_index("tp")
        core, x = tp % CORES, tp // CORES
        rows, width = tokens.shape
        ff = up_weight.shape[1] // n_grp
        block = down_weight.shape[1]

        up_own = lax.dynamic_slice_in_dim(up_weight, grp * ff, ff, 1).astype(jnp.bfloat16)
        down_own = lax.dynamic_slice_in_dim(down_weight, grp * ff, ff, 0).astype(jnp.bfloat16)
        scale_up = lax.dynamic_slice_in_dim(up_scale, grp * ff, ff, 0)

        everyone = [tokens] + [lax.ppermute(tokens, "grp", grp_shift(s)) for s in range(1, n_grp)]
        residual = tokens.astype(jnp.float32)
        normed = [rms_rows(t.astype(jnp.float32), pre_gain).astype(jnp.bfloat16) for t in everyone]
        normed = jnp.concatenate(normed, axis=0)

        up_n, down_n = pieces_of(ff), pieces_of(block)
        ups = [jnp.split(up_own, up_n, axis=1)]
        for _ in range(n_fs - 1):
            ups.append([lax.ppermute(u, "fs", ring) for u in ups[-1]])
        scales = [down_scale]
        for _ in range(n_fs - 1):
            scales.append(lax.ppermute(scales[-1], "fs", ring))
        downs = [jnp.split(down_own, down_n, axis=1)]
        first = [after(d, ups[-1][min(p, up_n - 1)]) for p, d in enumerate(downs[0])]
        for k in range(n_fs - 1):
            source = first if k == 0 else downs[-1]
            downs.append([lax.ppermute(d, "fs", ring) for d in source])

        hidden = []
        d_block = up_own.shape[0]
        for p in range(up_n):
            total = None
            for k in range(n_fs):
                left = lax.dynamic_slice_in_dim(normed, ((fs - k) % n_fs) * d_block, d_block, 1)
                term = jnp.dot(left, ups[k][p], preferred_element_type=jnp.float32)
                total = term if total is None else total + term
            part = lax.slice_in_dim(scale_up, p * (ff // up_n), (p + 1) * (ff // up_n))
            hidden.append(jnp.square(jax.nn.relu(total * part)).astype(jnp.bfloat16))
        hidden = jnp.concatenate(hidden, axis=1)

        half = rows // CORES

        def reduce(partial):
            partial = partial.reshape(n_grp, CORES, half, partial.shape[-1])
            keep = lax.dynamic_index_in_dim(partial, core, 1, keepdims=False)
            give = lax.dynamic_index_in_dim(partial, 1 - core, 1, keepdims=False)
            keep = keep + lax.ppermute(give.astype(jnp.bfloat16), "tp", swap_core).astype(jnp.float32)
            mine = keep[0]
            for s in range(1, n_grp):
                back = lax.ppermute(keep[s].astype(jnp.bfloat16), "grp", grp_shift(-s))
                mine = mine + back.astype(jnp.float32)
            mine = mine.astype(jnp.bfloat16)
            parts = [mine] + [lax.ppermute(mine, "tp", x_shift(s)) for s in range(1, n_x)]
            if n_x > 2:
                stacked = jnp.stack(parts)
                parts = [
                    lax.dynamic_index_in_dim(stacked, (x - i) % n_x, 0, keepdims=False)
                    for i in range(n_x)
                ]
            total = parts[0].astype(jnp.float32)
            for part in parts[1:]:
                total = total + part.astype(jnp.float32)
            total = total.astype(jnp.bfloat16)
            other = lax.ppermute(total, "tp", swap_core)
            return jnp.concatenate(
                [jnp.where(core == 0, total, other), jnp.where(core == 0, other, total)], axis=0
            )

        branch = jnp.zeros((rows, width), jnp.bfloat16)
        piece = block // down_n
        for k in range(n_fs):
            for p in range(down_n):
                out = jnp.dot(hidden, downs[k][p], preferred_element_type=jnp.float32)
                out = out * lax.slice_in_dim(scales[k], p * piece, (p + 1) * piece)
                at = ((fs - k) % n_fs) * block + p * piece
                branch = lax.dynamic_update_slice_in_dim(branch, reduce(out), at, 1)
        branch = branch.astype(jnp.float32)
        return (residual + rms_rows(branch, post_gain)).astype(jnp.bfloat16)

    placed = (P(("grp", "fs"), None), P(), P("fs", "tp"), P("tp"), P("tp", "fs"), P("fs"), P())
    return jax.shard_map(
        on_device, mesh=mesh, in_specs=placed, out_specs=P(("grp", "fs"), None), check_vma=False
    )
```

```python
import jax
import jax.numpy as jnp
from jax import lax
from jax.sharding import PartitionSpec as P

epsilon = 1e-06
CORES = 2


def rms_rows(values, scaling):
    return values * lax.rsqrt(jnp.mean(values * values, axis=-1, keepdims=True) + epsilon) * scaling


def pieces_of(width):
    return 2 if width % 256 == 0 else 1


def after(value, *earlier):
    return lax.optimization_barrier((value,) + earlier)[0]


def solution(mesh):
    n_grp, n_fs, n_tp = (mesh.shape[name] for name in ("grp", "fs", "tp"))
    n_x = n_tp // CORES
    ring = [(i, (i + 1) % n_fs) for i in range(n_fs)]
    swap_core = [(t, t ^ 1) for t in range(n_tp)]

    def fs_shift(s):
        return [(i, (i + s) % n_fs) for i in range(n_fs)]

    def grp_shift(s):
        return [(g, (g + s) % n_grp) for g in range(n_grp)]

    def x_shift(s):
        return [(t, (t + CORES * s) % n_tp) for t in range(n_tp)]

    def on_device(tokens, pre_gain, up_weight, up_scale, down_weight, down_scale, post_gain):
        grp, fs, tp = lax.axis_index("grp"), lax.axis_index("fs"), lax.axis_index("tp")
        core, x = tp % CORES, tp // CORES
        rows, width = tokens.shape
        ff = up_weight.shape[1] // n_grp
        block = down_weight.shape[1]

        up_own = lax.dynamic_slice_in_dim(up_weight, grp * ff, ff, 1).astype(jnp.bfloat16)
        down_own = lax.dynamic_slice_in_dim(down_weight, grp * ff, ff, 0).astype(jnp.bfloat16)
        scale_up = lax.dynamic_slice_in_dim(up_scale, grp * ff, ff, 0)

        everyone = [tokens] + [lax.ppermute(tokens, "grp", grp_shift(s)) for s in range(1, n_grp)]
        residual = tokens.astype(jnp.float32)
        normed = [rms_rows(t.astype(jnp.float32), pre_gain).astype(jnp.bfloat16) for t in everyone]
        normed = jnp.concatenate(normed, axis=0)

        scales = [down_scale] + [lax.ppermute(down_scale, "fs", fs_shift(k)) for k in range(1, n_fs)]
        up_own = after(up_own, *scales)

        up_n, down_n = pieces_of(ff), pieces_of(block)
        ups = [jnp.split(up_own, up_n, axis=1)]
        for _ in range(n_fs - 1):
            ups.append([lax.ppermute(u, "fs", ring) for u in ups[-1]])
        downs = [jnp.split(down_own, down_n, axis=1)]
        first = [after(d, ups[-2][min(p, up_n - 1)]) for p, d in enumerate(downs[0])]
        for k in range(n_fs - 1):
            source = first if k == 0 else downs[-1]
            downs.append([lax.ppermute(d, "fs", ring) for d in source])

        hidden = []
        d_block = up_own.shape[0]
        for p in range(up_n):
            total = None
            for k in range(n_fs):
                left = lax.dynamic_slice_in_dim(normed, ((fs - k) % n_fs) * d_block, d_block, 1)
                term = jnp.dot(left, ups[k][p], preferred_element_type=jnp.float32)
                total = term if total is None else total + term
            part = lax.slice_in_dim(scale_up, p * (ff // up_n), (p + 1) * (ff // up_n))
            hidden.append(jnp.square(jax.nn.relu(total * part)).astype(jnp.bfloat16))
        hidden = jnp.concatenate(hidden, axis=1)

        half = rows // CORES

        def reduce(partial):
            partial = partial.reshape(n_grp, CORES, half, partial.shape[-1])
            keep = lax.dynamic_index_in_dim(partial, core, 1, keepdims=False)
            give = lax.dynamic_index_in_dim(partial, 1 - core, 1, keepdims=False)
            keep = keep + lax.ppermute(give.astype(jnp.bfloat16), "tp", swap_core).astype(jnp.float32)
            mine = keep[0]
            for s in range(1, n_grp):
                back = lax.ppermute(keep[s].astype(jnp.bfloat16), "grp", grp_shift(-s))
                mine = mine + back.astype(jnp.float32)
            mine = mine.astype(jnp.bfloat16)
            parts = [mine] + [lax.ppermute(mine, "tp", x_shift(s)) for s in range(1, n_x)]
            if n_x > 2:
                stacked = jnp.stack(parts)
                parts = [
                    lax.dynamic_index_in_dim(stacked, (x - i) % n_x, 0, keepdims=False)
                    for i in range(n_x)
                ]
            total = parts[0].astype(jnp.float32)
            for part in parts[1:]:
                total = total + part.astype(jnp.float32)
            total = total.astype(jnp.bfloat16)
            other = lax.ppermute(total, "tp", swap_core)
            return jnp.concatenate(
                [jnp.where(core == 0, total, other), jnp.where(core == 0, other, total)], axis=0
            )

        branch = jnp.zeros((rows, width), jnp.bfloat16)
        piece = block // down_n
        for k in range(n_fs):
            for p in range(down_n):
                out = jnp.dot(hidden, downs[k][p], preferred_element_type=jnp.float32)
                out = out * lax.slice_in_dim(scales[k], p * piece, (p + 1) * piece)
                at = ((fs - k) % n_fs) * block + p * piece
                branch = lax.dynamic_update_slice_in_dim(branch, reduce(out), at, 1)
        branch = branch.astype(jnp.float32)
        return (residual + rms_rows(branch, post_gain)).astype(jnp.bfloat16)

    placed = (P(("grp", "fs"), None), P(), P("fs", "tp"), P("tp"), P("tp", "fs"), P("fs"), P())
    return jax.shard_map(
        on_device, mesh=mesh, in_specs=placed, out_specs=P(("grp", "fs"), None), check_vma=False
    )
```
